32 devices in a mesh: grp: 2 (over x), tp: 16 (over z, y, core).
Axes of the slice: x: 2, y: 2, z: 4, core: 2. Of those that a mesh axis runs over, the one named last changes fastest.
Arguments:
- tokens: bfloat16 [96, 4096], P('grp', 'tp'), parts along dimension 0, may hold values from -6 to 6
- states: float32 [2, 96, 32, 128, 128], P(None, 'grp', 'tp'), parts along dimension 1, may hold values from -10 to 10
- norm_gain: float32 [2, 4096], replicated, may hold values from 0.1 to 1.9
- query_weight: bfloat16 [2, 4096, 4096], P(None, None, 'tp'), may hold values from -0.09375 to 0.09375
- forget_weight: bfloat16 [2, 4096, 4096], P(None, None, 'tp'), may hold values from -0.09375 to 0.09375
- value_weight: bfloat16 [2, 4096, 4096], P(None, None, 'tp'), may hold values from -0.09375 to 0.09375
- gate_weight: bfloat16 [2, 4096, 4096], P(None, None, 'tp'), may hold values from -0.09375 to 0.09375
- output_weight: bfloat16 [2, 4096, 4096], P(None, 'tp'), may hold values from -0.125 to 0.125
- output_gain: float32 [2, 4096], P(None, 'tp'), may hold values from 0.1 to 1.9
- bound_logits: float32 [4096], P('tp'), may hold values from -6 to 6
Outputs:
- mixed: bfloat16 [96, 4096], P('grp', 'tp'), parts along dimension 0
- new_states: float32 [2, 96, 32, 128, 128], P(None, 'grp', 'tp'), parts along dimension 1
The draws below stay inside these ranges and needn't reach their ends.
There are 2 independent parts, one for each index of `grp`. The reference program is written for one: setup_inputs(seed, part) draws one part's arguments, and reference() takes and returns one part's arrays. A program takes and returns all parts, laid end to end along the dimension named above; an argument that names none is the same for every part. Nothing has to cross between parts.
All inputs are finite; a program needn't handle non-finite values.
Results may differ from the reference program's by a relative error of at most 0.017.
Values may be sent and summed in bfloat16 or wider, within the bound.
A program may use at most 128 MiB of HBM per device.

```python
import jax
import jax.numpy as jnp
from jax import lax

HEADS = 32
HEAD_DIM = 128
WIDTH = 4096
BATCH = 48


def draw_states(key, part):
    first_key = jax.random.fold_in(jax.random.fold_in(key, 17), 0)
    shape = (2, BATCH, HEADS, HEAD_DIM, HEAD_DIM)
    head_pos = jnp.arange(HEADS, dtype=jnp.float32) / (HEADS - 1)
    rising = 0.4 * jnp.power(6.0, head_pos)
    base = jnp.clip(jax.random.normal(first_key, shape, jnp.float32), -4.0, 4.0)
    return base * rising[None, None, :, None, None]


def with_spikes(entries, stream_key, source, target, parts, factor):
    owner, partner = [(jnp.arange(entries.shape[axis_at]) // (entries.shape[axis_at] // parts)).reshape([-1 if axis == axis_at else 1 for axis in range(entries.ndim)]) for axis_at in (source, target)]
    chosen = jax.random.permutation(stream_key, parts)[partner]
    strong = (owner == chosen) | (owner == (partner + parts // 2) % parts)
    return jnp.where(strong, factor * entries, entries)


def level_of(rng, dims, cuts, smallest, high):
    loudness, own = 1.0, jax.random.fold_in(rng, 6)
    for position, parts in cuts:
        draws = jnp.exp(jax.random.uniform(jax.random.fold_in(own, position), (parts,), jnp.float32, smallest / len(cuts), high / len(cuts)))
        loudness = loudness * jnp.repeat(draws, dims[position] // parts).reshape([-1 if axis == position else 1 for axis in range(len(dims))])
    return loudness


def scatter_about(own_key, extent, scale, reach, shards=(), held_as=jnp.bfloat16):
    result = jax.random.normal(own_key, extent, jnp.float32) * scale
    if len(shards) > 0:
        result = level_of(own_key, extent, shards, -0.22, 0.18) * result
    return jnp.clip(result, min=-reach, max=reach).astype(held_as)


def gaussian_with(key, dims, deviation, most, cuts, heavy, kind=jnp.bfloat16):
    entries = deviation * jax.random.normal(key, dims, jnp.float32)
    if cuts:
        entries = entries * level_of(key, dims, cuts, -0.22, 0.18)
    return jnp.clip(with_spikes(entries, jax.random.fold_in(key, 3), *heavy), -most, most).astype(kind)


def setup_inputs(seed: int = 0, part: int = 0) -> dict:
    arg_keys = jax.random.split(jax.random.key(seed), 11)
    part_keys = jax.random.split(jax.random.fold_in(arg_keys[10], part), 11)
    tokens = scatter_about(part_keys[0], (BATCH, WIDTH), 1.0, 6.0, ((1, 16),))
    states = draw_states(jax.random.fold_in(jax.random.fold_in(arg_keys[10], part), 71), part)
    norm_gain = jnp.clip(1.0 + 0.18 * jax.random.normal(arg_keys[2], (2, WIDTH), jnp.float32), 0.1, 1.9)
    query_weight = scatter_about(arg_keys[3], (2, WIDTH, WIDTH), WIDTH ** -0.5, 0.09375, ((2, 16),))
    forget_weight = scatter_about(arg_keys[4], (2, WIDTH, WIDTH), WIDTH ** -0.5, 0.09375, ((2, 16),))
    value_weight = scatter_about(arg_keys[5], (2, WIDTH, WIDTH), WIDTH ** -0.5, 0.09375, ((2, 16),))
    gate_weight = scatter_about(arg_keys[6], (2, WIDTH, WIDTH), WIDTH ** -0.5, 0.09375, ((2, 16),))
    output_weight = gaussian_with(arg_keys[7], (2, WIDTH, WIDTH), WIDTH ** -0.5, 0.125, ((1, 16),), (1, 2, 16, 2.0))
    output_gain = jnp.clip(1.0 + 0.18 * jax.random.normal(arg_keys[8], (2, WIDTH), jnp.float32), 0.1, 1.9)
    bound_logits = scatter_about(arg_keys[9], (WIDTH,), 1.5, 6.0, ((0, 16),), jnp.float32)
    return {"tokens": tokens, "states": states, "norm_gain": norm_gain, "query_weight": query_weight, "forget_weight": forget_weight, "value_weight": value_weight, "gate_weight": gate_weight, "output_weight": output_weight, "output_gain": output_gain, "bound_logits": bound_logits}


epsilon = 1e-06

def mixer_block(stream, state_in, gain_in, query_mat, forget_mat, value_mat, gate_mat, out_mat, gain_out, lower_bound):
    stream32 = stream.astype(jnp.float32)
    factor = lax.rsqrt(lax.optimization_barrier(jnp.mean(stream32 * stream32, axis=-1, keepdims=True)) + epsilon)
    normed = (stream32 * factor * gain_in).astype(jnp.bfloat16)
    query_proj = jnp.dot(normed, query_mat, preferred_element_type=jnp.float32).astype(jnp.bfloat16)
    forget_pre = jnp.dot(normed, forget_mat, preferred_element_type=jnp.float32).astype(jnp.bfloat16)
    value_proj = jnp.dot(normed, value_mat, preferred_element_type=jnp.float32).astype(jnp.bfloat16)
    gate_proj = jnp.dot(normed, gate_mat, preferred_element_type=jnp.float32).astype(jnp.bfloat16)
    forget = lower_bound + (1.0 - lower_bound) * jax.nn.sigmoid(forget_pre.astype(jnp.float32))
    rows = stream.shape[0]
    forget_heads = forget.reshape(rows, HEADS, HEAD_DIM)
    value_heads = value_proj.astype(jnp.float32).reshape(rows, HEADS, HEAD_DIM)
    query_heads = query_proj.astype(jnp.float32).reshape(rows, HEADS, HEAD_DIM) * HEAD_DIM ** (-0.5)
    updated = forget_heads[..., None] * state_in + (1.0 - forget_heads)[..., None] * value_heads[:, :, None, :]
    readout = jnp.einsum('bhk,bhkv->bhv', query_heads, updated, precision=lax.Precision.HIGHEST).reshape(rows, WIDTH)
    energy = lax.optimization_barrier(jnp.sum(readout * readout, axis=-1, keepdims=True))
    gated_rows = (readout * gain_out * jax.nn.silu(gate_proj.astype(jnp.float32))).astype(jnp.bfloat16)
    branch = jnp.dot(gated_rows, out_mat, preferred_element_type=jnp.float32) * lax.rsqrt(energy / WIDTH + epsilon)
    return ((stream32 + branch).astype(jnp.bfloat16), updated)

def reference(tokens, states, norm_gain, query_weight, forget_weight, value_weight, gate_weight, output_weight, output_gain, bound_logits):
    first, state_first = mixer_block(tokens, states[0], norm_gain[0], query_weight[0], forget_weight[0], value_weight[0], gate_weight[0], output_weight[0], output_gain[0], 0.0)
    mixed, state_second = mixer_block(first, states[1], norm_gain[1], query_weight[1], forget_weight[1], value_weight[1], gate_weight[1], output_weight[1], output_gain[1], jax.nn.sigmoid(bound_logits))
    return (mixed, jnp.stack([state_first, state_second]))
```

```python
import functools

import jax
import jax.numpy as jnp
from jax import lax
from jax.experimental import pallas as pl
from jax.experimental.pallas import tpu as pltpu
from jax.sharding import PartitionSpec as P

epsilon = 1e-06


def kernel(
    n,
    parts,
    tok,
    states,
    gain,
    wq,
    wf,
    wv,
    wg,
    wo,
    ogain,
    blog,
    mixed,
    new,
    w_s,
    wo_s,
    gain_s,
    ogain_s,
    blog_s,
    xg,
    acc,
    ss,
    tf,
    v_s,
    g_s,
    own,
    sb,
    ra,
    pb,
    rb,
    es,
    er,
    ep,
    eb,
    sm_sem,
    w_sem,
    gs,
    gr,
    fs,
    fr,
    asend,
    arecv,
    bsend,
    brecv,
    essend,
    esrecv,
    ebsend,
    ebrecv,
):
    rows, cols = tok.shape
    width = cols * n
    heads = states.shape[2]
    size = states.shape[3]
    part = rows // parts
    half = n // 2
    bunch = sb.shape[2] // arecv.shape[2]
    f32, b16 = jnp.float32, jnp.bfloat16
    me = lax.axis_index("tp")
    core = lax.rem(me, 2)
    chip = me // 2
    sib = me + 1 - 2 * core

    def other(s):
        found, bit = 0, 1
        while bit < half:
            found = found + bit * ((chip // bit + s // bit) % 2)
            bit *= 2
        return found

    def peer(s):
        return 2 * other(s) + core

    def sib_peer(s):
        return 2 * other(s) + 1 - core

    def span(d):
        return pl.ds(pl.multiple_of(d * cols, cols), cols)

    def lines(p):
        return pl.ds(p * part, part)

    def remote(src, dst, send, recv, d):
        return pltpu.make_async_remote_copy(
            src_ref=src,
            dst_ref=dst,
            send_sem=send,
            recv_sem=recv,
            device_id={"tp": d},
            device_id_type=pl.DeviceIdType.MESH,
        )

    barrier = pltpu.get_barrier_semaphore()

    def greet(d):
        pl.semaphore_signal(
            barrier, inc=1, device_id={"tp": d}, device_id_type=pl.DeviceIdType.MESH
        )

    @pl.loop(1, half)
    def _(t):
        greet(peer(half - t))

    greet(sib)

    tok_copy = pltpu.make_async_copy(tok, xg.at[0, me], sm_sem.at[0])
    tok_copy.start()
    gain_copy = pltpu.make_async_copy(gain, gain_s, sm_sem.at[1])
    gain_copy.start()
    og_copy = pltpu.make_async_copy(ogain, ogain_s, sm_sem.at[2])
    og_copy.start()
    bl_copy = pltpu.make_async_copy(blog, blog_s, sm_sem.at[3])
    bl_copy.start()

    def weight_copies(l):
        return [
            pltpu.make_async_copy(w.at[l], w_s.at[l, i], w_sem.at[l, i])
            for i, w in enumerate((wq, wf, wv, wg))
        ]

    def later_copies(l):
        return [
            pltpu.make_async_copy(states.at[l], new.at[l], w_sem.at[l, 4]),
            pltpu.make_async_copy(wo.at[l], wo_s.at[l], w_sem.at[l, 5]),
        ]

    for c in weight_copies(0):
        c.start()
    tok_copy.wait()
    pl.semaphore_wait(barrier, half)

    def gather_copy(l, s):
        return remote(xg.at[l, me], xg.at[l, me], gs.at[l], gr.at[l, s], peer(s))

    def gather_part(l, p, s):
        ref = xg.at[l, me, lines(p)]
        return remote(ref, ref, gs.at[l], gr.at[l, s], peer(s))

    def forward_copy(l, s):
        o = peer(s)
        return remote(xg.at[l, o], xg.at[l, o], fs.at[l], fr.at[l, s], sib)

    def a_copy(l, p, c):
        block = pl.ds(c * bunch, bunch)
        return remote(
            sb.at[l, p, block],
            ra.at[l, p, block],
            asend.at[l],
            arecv.at[l, p, c],
            sib,
        )

    def b_copy(l, p, i):
        d = peer(half - 1 - i)
        return remote(
            pb.at[l, p, i], rb.at[l, p, i], bsend.at[l], brecv.at[l, p], d
        )

    def es_copy(l, p):
        return remote(
            es.at[l, p], er.at[l, p], essend.at[l, p], esrecv.at[l, p], sib
        )

    def eb_copy(l, p, i):
        d = peer(half - 1 - i)
        return remote(ep.at[l, p], eb.at[l, p, i], ebsend.at[l], ebrecv.at[l, p], d)

    row_of = lax.broadcasted_iota(jnp.int32, (part, 128), 0)
    diagonal = row_of == lax.broadcasted_iota(jnp.int32, (part, 128), 1)

    @pl.loop(1, half)
    def _(t):
        gather_copy(0, half - t).start()

    forward_copy(0, 0).start()

    for l in range(2):
        acc[...] = jnp.zeros_like(acc)
        ss[...] = jnp.zeros_like(ss)

        def chunk(o):
            x = xg[l, o].astype(f32)
            square = x * x
            total = square[:, :128]
            for c in range(128, cols, 128):
                total = total + square[:, c : c + 128]
            ss[...] += total
            scaled = (x * gain_s[l : l + 1, span(o)]).astype(b16)
            for i in range(4):
                acc[i] += jnp.dot(
                    scaled, w_s[l, i, span(o), :], preferred_element_type=f32
                )

        if l == 0:
            gain_copy.wait()
        for c in weight_copies(l):
            c.wait()
        if l == 0:
            for c in later_copies(0):
                c.start()
        chunk(me)
        forward_copy(l, 0).wait_recv()
        chunk(sib)

        @pl.loop(1, half)
        def _(s):
            gather_copy(l, s).wait_recv()
            forward_copy(l, s).start()
            chunk(peer(s))

        @pl.loop(1, half)
        def _(s):
            forward_copy(l, s).wait_recv()
            chunk(sib_peer(s))

        factor = lax.rsqrt(jnp.sum(ss[...], axis=-1, keepdims=True) / width + epsilon)

        def projected(i):
            return (acc[i] * factor).astype(b16).astype(f32)

        if l == 0:
            og_copy.wait()
            bl_copy.wait()
        query = projected(0) * size**-0.5
        forget = jax.nn.sigmoid(projected(1))
        if l == 1:
            lower = jax.nn.sigmoid(blog_s[...])
            forget = lower + (1.0 - lower) * forget
        value = projected(2)
        v_s[...] = value
        kept = query * forget
        fresh = query - kept
        gate = ogain_s[l : l + 1, :] * jax.nn.silu(projected(3))
        pad = jnp.zeros((size - rows, size), f32)
        state_copy, wo_copy = later_copies(l)
        state_copy.wait()
        wo_copy.wait()
        if l == 0:
            for c in weight_copies(1) + later_copies(1):
                c.start()

        for p in range(parts):
            here = slice(p * part, (p + 1) * part)
            reads = []
            for h in range(heads):
                lanes = slice(h * size, (h + 1) * size)
                asked = kept[here, lanes]
                spread = jnp.concatenate(
                    [
                        jnp.where(row_of == j, asked, 0.0).astype(b16)
                        for j in range(part)
                    ],
                    axis=1,
                )
                held = new[l, here, h].reshape(part * size, size).astype(b16)
                old = jnp.dot(spread, held, preferred_element_type=f32)
                share = jnp.sum(fresh[here, lanes], axis=-1, keepdims=True)
                reads.append(old + share * value[here, lanes])
            readout = jnp.concatenate(reads, axis=1)
            energy = jnp.sum(readout * readout, axis=-1, keepdims=True)
            es[l, p] = jnp.sum(
                jnp.where(diagonal, energy, 0.0), axis=0, keepdims=True
            )
            es_copy(l, p).start()
            g_s[here, :] = (readout * gate[here, :]).astype(b16)

            def product(d):
                return jnp.dot(
                    g_s[here, :], wo_s[l, :, span(d)], preferred_element_type=f32
                )

            @pl.loop(0, half // bunch)
            def _(c):
                for k in range(bunch):
                    i = c * bunch + k
                    sb[l, p, i] = product(sib_peer(half - 1 - i)).astype(b16)
                a_copy(l, p, c).start()

            es_copy(l, p).wait_recv()
            ep[l, p] = es[l, p] + er[l, p]

            @pl.loop(0, half // bunch)
            def _(c):
                mine = [
                    product(peer(half - 1 - c * bunch - k)) for k in range(bunch)
                ]
                a_copy(l, p, c).wait_recv()
                for k in range(bunch):
                    i = c * bunch + k
                    both = mine[k] + ra[l, p, i].astype(f32)
                    if k < bunch - 1:
                        pb[l, p, i] = both.astype(b16)
                        b_copy(l, p, i).start()
                        eb_copy(l, p, i).start()
                    else:
                        own[p] = both

                        @pl.when(c < half // bunch - 1)
                        def _():
                            pb[l, p, i] = own[p].astype(b16)
                            b_copy(l, p, i).start()
                            eb_copy(l, p, i).start()

        for h in range(heads):
            lane = slice(h * size, (h + 1) * size)
            flipped = jnp.concatenate([forget[:, lane], pad], axis=0).T
            for b in range(rows // 8):
                shift = (size - 8 * b) % size
                tf[b, h] = pltpu.roll(flipped, shift, 1) if shift else flipped

        def update(first, last):
            @pl.loop(first, last)
            def _(b):
                base = pl.multiple_of(b * 8, 8)
                for h in range(heads):
                    values = v_s[pl.ds(base, 8), h * size : (h + 1) * size]
                    for j in range(8):
                        line = values[j : j + 1, :]
                        keep = tf[b, h, :, j : j + 1]
                        new[l, base + j, h] = (
                            keep * (new[l, base + j, h] - line) + line
                        )

        if l == 1:
            update(0, rows // 8)

        for p in range(parts):
            here = slice(p * part, (p + 1) * part)
            remote(
                ep.at[l, p], eb.at[l, p], ebsend.at[l], ebrecv.at[l, p], sib
            ).wait_recv()
            powers = ep[l, p]
            for i in range(half - 1):
                powers = powers + eb[l, p, i]
            column = jnp.sum(
                jnp.where(diagonal, powers, 0.0), axis=1, keepdims=True
            )
            rescale = lax.rsqrt(column / width + epsilon)
            remote(
                pb.at[l, p], rb.at[l, p], bsend.at[l], brecv.at[l, p], sib
            ).wait_recv()
            total = own[p]
            for i in range(half - 1):
                total = total + rb[l, p, i].astype(f32)
            stream = (xg[l, me, here].astype(f32) + total * rescale).astype(b16)
            if l == 0:
                xg[1, me, here] = stream

                @pl.loop(1, half)
                def _(t):
                    gather_part(1, p, half - t).start()

                if p == parts - 1:
                    forward_copy(1, 0).start()
                update(p * part // 8, (p + 1) * part // 8)
            else:
                mixed[here, :] = stream

    for l in range(2):
        remote(
            xg.at[l, pl.ds(0, half - 1)],
            xg.at[l, pl.ds(0, half - 1)],
            gs.at[l],
            gr.at[l, 0],
            sib,
        ).wait_send()
        remote(
            xg.at[l, pl.ds(0, half)],
            xg.at[l, pl.ds(0, half)],
            fs.at[l],
            fr.at[l, 0],
            sib,
        ).wait_send()
        remote(sb.at[l], ra.at[l], asend.at[l], arecv.at[l, 0, 0], sib).wait_send()
        remote(pb.at[l], rb.at[l], bsend.at[l], brecv.at[l, 0], sib).wait_send()
        remote(eb.at[l], eb.at[l], ebsend.at[l], ebrecv.at[l, 0], sib).wait_send()
        for p in range(parts):
            es_copy(l, p).wait_send()


def body(
    n,
    tokens,
    states,
    norm_gain,
    query_weight,
    forget_weight,
    value_weight,
    gate_weight,
    output_weight,
    output_gain,
    bound_logits,
):
    rows, cols = tokens.shape
    width = cols * n
    heads, size = states.shape[2:4]
    groups = rows // 8
    half = n // 2
    bunch = 4
    parts = rows // 16
    part = rows // parts
    f32, b16 = jnp.float32, jnp.bfloat16
    dma = pltpu.SemaphoreType.DMA
    anywhere = pl.BlockSpec(memory_space=pl.ANY)
    in_vmem = pl.BlockSpec(memory_space=pltpu.VMEM)
    mixed, new = pl.pallas_call(
        functools.partial(kernel, n, parts),
        out_shape=(
            jax.ShapeDtypeStruct(tokens.shape, b16),
            pltpu.VMEM(states.shape, f32),
        ),
        in_specs=[anywhere] * 10,
        out_specs=(in_vmem, in_vmem),
        scratch_shapes=[
            pltpu.VMEM((2, 4, width, cols), b16),
            pltpu.VMEM((2, cols, width), b16),
            pltpu.VMEM((2, width), f32),
            pltpu.VMEM((2, cols), f32),
            pltpu.VMEM((1, cols), f32),
            pltpu.VMEM((2, n, rows, cols), b16),
            pltpu.VMEM((4, rows, cols), f32),
            pltpu.VMEM((rows, 128), f32),
            pltpu.VMEM((groups, heads, size, size), f32),
            pltpu.VMEM((rows, cols), f32),
            pltpu.VMEM((rows, cols), b16),
            pltpu.VMEM((parts, part, cols), f32),
            pltpu.VMEM((2, parts, half, part, cols), b16),
            pltpu.VMEM((2, parts, half, part, cols), b16),
            pltpu.VMEM((2, parts, half - 1, part, cols), b16),
            pltpu.VMEM((2, parts, half - 1, part, cols), b16),
            pltpu.VMEM((2, parts, 1, 128), f32),
            pltpu.VMEM((2, parts, 1, 128), f32),
            pltpu.VMEM((2, parts, 1, 128), f32),
            pltpu.VMEM((2, parts, half - 1, 1, 128), f32),
            dma((4,)),
            dma((2, 6)),
            dma((2,)),
            dma((2, half)),
            dma((2,)),
            dma((2, half)),
            dma((2,)),
            dma((2, parts, half // bunch)),
            dma((2,)),
            dma((2, parts)),
            dma((2, parts)),
            dma((2, parts)),
            dma((2,)),
            dma((2, parts)),
        ],
        compiler_params=pltpu.CompilerParams(
            collective_id=0, has_side_effects=True, vmem_limit_bytes=46000 * 1024
        ),
    )(
        tokens,
        states,
        norm_gain,
        query_weight,
        forget_weight,
        value_weight,
        gate_weight,
        output_weight,
        output_gain,
        bound_logits.reshape(1, cols),
    )
    return mixed, new


def solution(mesh):
    placed = (
        P("grp", "tp"),
        P(None, "grp", "tp", None, None),
        P(),
        P(None, None, "tp"),
        P(None, None, "tp"),
        P(None, None, "tp"),
        P(None, None, "tp"),
        P(None, "tp", None),
        P(None, "tp"),
        P("tp"),
    )
    return jax.shard_map(
        functools.partial(body, mesh.shape["tp"]),
        mesh=mesh,
        in_specs=placed,
        out_specs=(P("grp", "tp"), P(None, "grp", "tp", None, None)),
        check_vma=False,
    )
```
